32 devices in a mesh: ep: 8 (over z, x), tp: 4 (over y, core).
Axes of the slice: x: 2, y: 2, z: 4, core: 2. Of those that a mesh axis runs over, the one named last changes fastest.
Arguments:
- tokens: bfloat16 [256, 2048], P('ep'), may hold values from -6 to 6
- norm_gain: float32 [2048], replicated, may hold values from 0.1 to 1.9
- norm_bias: float32 [2048], replicated, may hold values from -3 to 3
- routes: int32 [256, 4], P('ep'), may hold values from 0 to 7, all different within a row; in each aligned block of 32 rows (0 to 31, 32 to 63, ...) at most 32 rows name the same one
- route_weights: float32 [256, 4], P('ep'), may hold values from 0.2 to 1
- gate_w: bfloat16 [8, 2048, 4096], P('ep', None, 'tp'), may hold values from -0.125 to 0.125
- up_w: bfloat16 [8, 2048, 4096], P('ep', None, 'tp'), may hold values from -0.125 to 0.125
- down_w: bfloat16 [8, 4096, 2048], P('ep', 'tp'), may hold values from -0.09375 to 0.09375
Outputs:
- mixed: bfloat16 [256, 2048], P('ep', 'tp')
The draws below stay inside these ranges and needn't reach their ends.
Inputs may be any that keep to these rules, and one draw needn't show every extreme that they name: `routes`: the 4 experts of a token differ; the rows of one index of ep name no expert more than 32 times, and in every draw some index of ep names some expert exactly 32 times.
All inputs are finite; a program needn't handle non-finite values.
Results may differ from the reference program's by a relative error of at most 0.017.
Values may be sent and summed in bfloat16 or wider, within the bound.
No kernel may reach another device: no remote copies, remote signals or barrier semaphores. Data moves between devices by JAX's collectives and lax.ppermute only.
A program may use at most 64 MiB of HBM per device.

```python
import math
import jax
import jax.numpy as jnp
import numpy as np
from jax import lax

D = 2048
FF = 4096
TOPK = 4
TOK_DEV = 32
EXPERTS = 8
CAP = 32
TOKENS = 256
N_TP = 4


def block_scale(rng, dims, shards, smallest, top_value):
    def one(position, parts):
        heights = jax.random.uniform(jax.random.fold_in(jax.random.fold_in(rng, 6), position), (parts,), jnp.float32, smallest / len(shards), top_value / len(shards))
        return jnp.repeat(jnp.exp(heights), dims[position] // parts).reshape((-1,) + (1,) * (len(dims) - position - 1))

    level = one(*shards[0])
    for cut in shards[1:]:
        level = level * one(*cut)
    return level


def deal_out(own_key, own, number, rows, number_of, top, bound, lean):
    sequence = jax.random.permutation(own_key, number_of)
    crowded, common = shares(number_of, rows * top, bound, lean, True), shares(number_of, rows * top, bound, lean, False)
    places = jnp.arange(number_of)

    def named(tallies, turn):
        used = int((tallies > 0).sum())
        fixed = max(1, used // 4)
        moved = fixed + (places - fixed + turn * (used - fixed)) % max(1, number_of - fixed)
        return jnp.zeros((number_of,), jnp.int32).at[sequence[jnp.where(places < fixed, places, moved)]].set(jnp.asarray(tallies, jnp.int32))

    tallies = jnp.where(number % 4 == 0, named(crowded, number // 4), named(common, number - number // 4 - 1))
    mixed = jax.random.permutation(jax.random.fold_in(own, 3), number_of)
    donor, sink = mixed[0:number_of // 2 * 2:2], mixed[1:number_of // 2 * 2:2]
    slack = jnp.minimum(tallies[donor] - 1, bound - tallies[sink]) // 2
    slack = jnp.where((donor == sequence[0]) | (sink == sequence[0]) | (tallies[sink] == 0), 0, jnp.maximum(slack, 0))
    moved = jax.random.randint(jax.random.fold_in(own, 4), (number_of // 2,), 0, 1 << 20) % (slack + 1)
    tallies = tallies.at[donor].add(-moved).at[sink].add(moved)
    labels = jnp.searchsorted(jnp.cumsum(tallies), jnp.arange(rows * top), side="right").astype(jnp.int32)
    listing = labels.reshape(top, rows).T
    listing = listing[jax.random.permutation(jax.random.fold_in(own, 1), rows)]
    turn = jax.random.randint(jax.random.fold_in(own, 2), (rows, 1), 0, top)
    return jnp.take_along_axis(listing, (jnp.arange(top)[None, :] + turn) % top, axis=1)


def shares(count, total, reach, slope, full):
    portions = [(1 << 20) // math.isqrt(rank ** slope) + 1 for rank in range(1, count + 1)]
    largest = reach if full else min(reach, max(-(-total // count), total * portions[0] // sum(portions)))
    least = 1 if total - largest >= count - 1 else 0
    counts, rest = [largest] + [least] * (count - 1), total - largest - least * (count - 1)
    while rest > 0:
        candidates = [i for i in range(1, count) if counts[i] < largest] or [i for i in range(1, count) if counts[i] < reach]
        pool, budget = sum([portions[i] for i in candidates]), rest
        for i in candidates:
            more = min(reach - counts[i], max(1, budget * portions[i] // pool), rest)
            counts[i] = counts[i] + more
            rest = rest - more
    return np.array(counts)


def scatter_about(own_key, shape, spread, most, shards=(), held_as=jnp.bfloat16):
    level = block_scale(own_key, shape, shards, -0.22, 0.18) if shards else 1.0
    drawn = jax.random.normal(own_key, shape, jnp.float32) * spread * level
    return jnp.minimum(jnp.maximum(drawn, -most), most).astype(held_as)


def setup_inputs(seed: int = 0) -> dict:
    splits = jax.random.split(jax.random.key(seed), 9)
    tokens = scatter_about(splits[0], (TOKENS, D), 1.0, 6.0, ((0, 8),))
    norm_gain = jnp.clip(1.0 + 0.18 * jax.random.normal(splits[1], (D,), jnp.float32), 0.1, 1.9)
    norm_bias = scatter_about(splits[2], (D,), 0.5, 3.0, (), jnp.float32)
    routes_keys = jax.random.split(jax.random.fold_in(splits[3], 1), TOKENS // TOK_DEV)
    routes_turns = jax.random.permutation(jax.random.fold_in(splits[3], 3), TOKENS // TOK_DEV)
    routes = jax.vmap(lambda own, number: deal_out(jax.random.fold_in(splits[3], 2), own, number, TOK_DEV, EXPERTS, TOPK, CAP, 2))(routes_keys, routes_turns).reshape((TOKENS, TOPK))
    route_weights = jnp.clip(0.2 + 0.8 * jax.random.uniform(splits[4], (TOKENS, TOPK), jnp.float32) ** block_scale(splits[4], (TOKENS, TOPK), ((0, 8),), -0.2, 0.2), 0.2, 1.0)
    gate_w = scatter_about(splits[5], (EXPERTS, D, FF), D ** -0.5, 0.125, ((0, 8), (2, 4)))
    up_w = scatter_about(splits[6], (EXPERTS, D, FF), D ** -0.5, 0.125, ((0, 8), (2, 4)))
    down_w = scatter_about(splits[7], (EXPERTS, FF, D), FF ** -0.5, 0.09375, ((0, 8), (1, 4)))
    return {"tokens": tokens, "norm_gain": norm_gain, "norm_bias": norm_bias, "routes": routes, "route_weights": route_weights, "gate_w": gate_w, "up_w": up_w, "down_w": down_w}


def layer_norm(tokens, norm_gain, norm_bias):
    values = tokens.astype(jnp.float32)
    centred = values - lax.optimization_barrier(jnp.mean(values, axis=-1, keepdims=True))
    variance = lax.optimization_barrier(jnp.mean(centred * centred, axis=-1, keepdims=True))
    return (centred * lax.rsqrt(variance + 1e-05) * norm_gain + norm_bias).astype(jnp.bfloat16)

def reference(tokens, norm_gain, norm_bias, routes, route_weights, gate_w, up_w, down_w):
    normed = layer_norm(tokens, norm_gain, norm_bias)
    groups = N_TP
    width = down_w.shape[2]
    hidden_units = down_w.shape[1]

    def one_expert(weights):
        gate_one, up_one, down_one = weights
        gate = jnp.dot(normed, gate_one, preferred_element_type=jnp.float32)
        up = jnp.dot(normed, up_one, preferred_element_type=jnp.float32)
        hidden = (jax.nn.silu(gate) * up).astype(jnp.bfloat16)
        hidden_groups = hidden.reshape(hidden.shape[0], groups, hidden_units // groups).astype(jnp.float32)
        down_groups = down_one.reshape(groups, hidden_units // groups, width).astype(jnp.float32)
        partial_sums = jnp.einsum('tgf,gfd->gtd', hidden_groups, down_groups).astype(jnp.bfloat16)
        return lax.optimization_barrier(jnp.sum(partial_sums.astype(jnp.float32), axis=0)).astype(jnp.bfloat16)
    expert_out = lax.map(one_expert, (gate_w, up_w, down_w))
    rows = jnp.arange(tokens.shape[0], dtype=jnp.int32)[:, None]
    chosen = expert_out[routes, rows].astype(jnp.float32)
    return lax.optimization_barrier(jnp.sum(route_weights[:, :, None] * chosen, axis=1)).astype(jnp.bfloat16)
```

```python
import functools

import jax
import jax.numpy as jnp
from jax import lax
from jax.experimental import pallas as pl
from jax.experimental.pallas import tpu as pltpu
from jax.sharding import PartitionSpec as P


AXES = ("ep", "tp")
CORES = 2
LANES = 128


class Grid:
    def __init__(self, ep, tp):
        self.y = tp // CORES
        self.x = self.y
        self.z = ep // self.x
        assert self.z * self.x == ep and self.y * CORES == tp
        self.devices = ep * tp

    def place(self, device):
        rest, core = divmod(device, CORES)
        rest, y = divmod(rest, self.y)
        z, x = divmod(rest, self.x)
        return z, x, y, core

    def device(self, z, x, y, core):
        return ((z * self.x + x) * self.y + y) * CORES + core

    def permute(self, value, moves):
        pairs = []
        for source in range(self.devices):
            here = self.place(source)
            move = moves[here[3]]
            if move is not None:
                pairs.append((source, self.device(*(a ^ b for a, b in zip(here, move)))))
        return lax.ppermute(value, AXES, pairs)


def in_hbm(value):
    return pltpu.with_memory_space_constraint(value, pltpu.HBM)


def fetch_kernel(*refs):
    count = len(refs) // 2
    sems = refs[-1]
    copies = [pltpu.make_async_copy(refs[i], refs[count + i], sems.at[i]) for i in range(count)]
    for copy in copies:
        copy.start()
    for copy in copies:
        copy.wait()


def prepare_kernel(*refs):
    out_ref, sems = refs[5], refs[11]
    copies = [pltpu.make_async_copy(refs[i], refs[6 + i], sems.at[i]) for i in range(5)]
    for copy in copies:
        copy.start()
    for copy in copies:
        copy.wait()
    tokens_ref, gain_ref, bias_ref, routes_ref, weights_ref = refs[6:11]
    values = tokens_ref[...].astype(jnp.float32)
    rows, width = values.shape
    centred = values - jnp.mean(values, axis=-1, keepdims=True)
    variance = jnp.mean(centred * centred, axis=-1, keepdims=True)
    normed = centred * lax.rsqrt(variance + 1e-05) * gain_ref[...] + bias_ref[...]
    out_ref[:, :width] = normed.astype(jnp.bfloat16)
    half = LANES // 2
    expert = lax.broadcasted_iota(jnp.int32, (half, rows), 0)
    total = jnp.zeros((half, rows), jnp.float32)
    for k in range(routes_ref.shape[0]):
        total += jnp.where(routes_ref[k : k + 1, :] == expert, weights_ref[k : k + 1, :], 0.0)
    high = total.astype(jnp.bfloat16)
    low = (total - high.astype(jnp.float32)).astype(jnp.bfloat16)
    lane = lax.broadcasted_iota(jnp.int32, (half, LANES), 1)
    line = lax.broadcasted_iota(jnp.int32, (half, LANES), 0)
    marks = jnp.zeros((rows, LANES), jnp.float32)
    for value, shift in ((high, 0), (low, half)):
        spread = (lane == line + shift).astype(jnp.bfloat16)
        marks += lax.dot_general(
            value, spread, (((0,), (0,)), ((), ())), preferred_element_type=jnp.float32
        )
    out_ref[:, width:] = marks.astype(jnp.bfloat16)


def expert_kernel(grid, pairs, chunk, *refs):
    count = 1 + 2 * len(pairs)
    blocks = refs[:count]
    gate_ref, up_ref, down_ref, keep_ref, send_ref, rows_ref, hidden_ref = refs[count:]
    width, units = gate_ref.shape[1:]
    columns = keep_ref.shape[-1]
    tok_rows = blocks[0].shape[0]

    core = lax.axis_index("tp") % CORES
    expert = lax.axis_index("ep")
    spare = grid.z * grid.x

    def slot(message):
        return spare if message is None else message[1] * grid.z + message[0]

    def place(block, at):
        start = pl.multiple_of(at * tok_rows, tok_rows)
        rows_ref[pl.ds(start, tok_rows), :] = block[...]

    place(blocks[0], 0)
    for i, (first, second) in enumerate(pairs):
        place(blocks[1 + 2 * i], jnp.where(core == 0, slot(first), slot(second)))
        place(blocks[2 + 2 * i], jnp.where(core == 0, slot(second), slot(first)))

    total_rows = spare * tok_rows
    for step in range(units // chunk):
        part = slice(step * chunk, (step + 1) * chunk)
        normed = rows_ref[:total_rows, :width]
        gate = jnp.dot(normed, gate_ref[0, :, part], preferred_element_type=jnp.float32)
        up = jnp.dot(normed, up_ref[0, :, part], preferred_element_type=jnp.float32)
        hidden_ref[:, part] = (gate / (1.0 + jnp.exp(-gate)) * up).astype(jnp.bfloat16)

    marks = rows_ref[:total_rows, width:].astype(jnp.float32)
    lane = lax.broadcasted_iota(jnp.int32, marks.shape, 1)
    mine = (lane == expert) | (lane == expert + LANES // 2)
    scale = jnp.sum(jnp.where(mine, marks, 0.0), axis=-1, keepdims=True)

    side = grid.z * tok_rows
    for y in range(grid.y):
        for c in range(CORES):
            owner = lax.axis_index("tp") ^ (y * CORES + c)
            start = pl.multiple_of(owner * columns, columns)
            part = jnp.dot(
                hidden_ref[...],
                down_ref[0, :, pl.ds(start, columns)],
                preferred_element_type=jnp.float32,
            )
            part = (part * scale).astype(jnp.bfloat16)
            target = send_ref if c else keep_ref
            y_first = core == c
            for x in range(grid.x):
                a = jnp.where(y_first, y, x)
                b = jnp.where(y_first, x, y)
                target[a, b] = part[x * side : (x + 1) * side]


def body(grid, tokens, norm_gain, norm_bias, routes, route_weights, gate_w, up_w, down_w):
    tok_rows, width = tokens.shape
    experts = lax.axis_size("ep")
    units = gate_w.shape[2]
    columns = width // lax.axis_size("tp")
    sources = (tokens, norm_gain[None, :], norm_bias[None, :], routes.T, route_weights.T)
    block = pl.pallas_call(
        prepare_kernel,
        out_shape=jax.ShapeDtypeStruct((tok_rows, width + LANES), jnp.bfloat16),
        in_specs=[pl.BlockSpec(memory_space=pltpu.HBM)] * 5,
        out_specs=pl.BlockSpec(memory_space=pltpu.VMEM),
        scratch_shapes=[pltpu.VMEM(a.shape, a.dtype) for a in sources]
        + [pltpu.SemaphoreType.DMA((5,))],
        compiler_params=pltpu.CompilerParams(vmem_limit_bytes=4 << 20),
        name="prepare",
    )(*map(in_hbm, sources))

    direct = [(z, 0) for z in range(2, grid.z)] + [(1, 0)] * (grid.z > 1)
    direct += [(0, x) for x in range(1, grid.x)]
    direct += [(1, x) for x in range(1, grid.x)] * (grid.z > 1)
    onward = [(z, x) for x in range(1, grid.x) for z in range(2, grid.z)]
    pairs, got = [], []
    for messages in (direct, onward):
        for first, second in zip(messages[::2], messages[1::2] + [None] * (len(messages) % 2)):
            pair = (first, second)
            if messages is direct:
                got.append(grid.permute(block, [m and (*m, 0, 0) for m in pair]))
            else:
                held = got[pairs.index(((first[0], 0), second and (second[0], 0)))]
                got.append(grid.permute(held, [m and (0, m[1], 0, 0) for m in pair]))
            pairs.append(pair)
    blocks = [block]
    for held in got:
        blocks += [held, grid.permute(held, [(0, 0, 0, 1)] * CORES)]

    weights = (gate_w, up_w, down_w)
    load = pl.pallas_call(
        fetch_kernel,
        out_shape=[pltpu.VMEM(w.shape, w.dtype) for w in weights],
        in_specs=[pl.BlockSpec(memory_space=pltpu.HBM)] * len(weights),
        out_specs=[pl.BlockSpec(memory_space=pltpu.VMEM)] * len(weights),
        scratch_shapes=[pltpu.SemaphoreType.DMA((len(weights),))],
        compiler_params=pltpu.CompilerParams(vmem_limit_bytes=1 << 20),
        name="fetch",
    )
    gate_w, up_w, down_w = load(*map(in_hbm, weights))

    rows = experts * tok_rows
    chunk = 256
    shape = (grid.y, grid.x, grid.z * tok_rows, columns)
    keep, send = pl.pallas_call(
        functools.partial(expert_kernel, grid, pairs, chunk),
        out_shape=[jax.ShapeDtypeStruct(shape, jnp.bfloat16)] * 2,
        in_specs=[pl.BlockSpec(memory_space=pltpu.VMEM)] * (len(blocks) + 3),
        out_specs=[pl.BlockSpec(memory_space=pltpu.VMEM)] * 2,
        scratch_shapes=[
            pltpu.VMEM((rows + tok_rows, width + LANES), jnp.bfloat16),
            pltpu.VMEM((rows, units), jnp.bfloat16),
        ],
        compiler_params=pltpu.CompilerParams(vmem_limit_bytes=24 << 20),
        name="expert",
    )(*blocks, gate_w, up_w, down_w)

    def add(*parts):
        total = parts[0].astype(jnp.float32)
        for part in parts[1:]:
            total = total + part.astype(jnp.float32)
        return total.astype(jnp.bfloat16)

    held = add(keep, grid.permute(send, [(0, 0, 0, 1)] * CORES))
    held = add(
        held[0],
        *(grid.permute(held[i], [(0, 0, i, 0), (0, i, 0, 0)]) for i in range(1, grid.y)),
    )
    held = add(
        held[0],
        *(grid.permute(held[i], [(0, i, 0, 0), (0, 0, i, 0)]) for i in range(1, grid.x)),
    )
    held = held.reshape(grid.z, tok_rows, columns)
    return add(
        held[0],
        *(grid.permute(held[i], [(i, 0, 0, 0)] * CORES) for i in range(1, grid.z)),
    )


def solution(mesh):
    grid = Grid(mesh.shape["ep"], mesh.shape["tp"])
    placed = (
        P("ep", None),
        P(),
        P(),
        P("ep", None),
        P("ep", None),
        P("ep", None, "tp"),
        P("ep", None, "tp"),
        P("ep", "tp", None),
    )
    return jax.shard_map(
        functools.partial(body, grid),
        mesh=mesh,
        in_specs=placed,
        out_specs=P("ep", "tp"),
        check_vma=False,
    )
```
